32 devices in a mesh: kv: 4 (over y, x), tp: 8 (over z, core).
Axes of the slice: x: 2, y: 2, z: 4, core: 2. Of those that a mesh axis runs over, the one named last changes fastest.
Arguments:
- tokens: bfloat16 [64, 4096], P(None, ('kv', 'tp')), may hold values from -6 to 6
- memory: float32 [64, 16, 256, 128], P('kv', 'tp'), may hold values from -6 to 6
- normalizer: float32 [64, 16, 128], P('kv', 'tp'), may hold values from -6 to 6
- stabilizer: float32 [64, 16], P('kv', 'tp'), may hold values from -4 to 4
- first_gain: float32 [4096], replicated, may hold values from 0.1 to 1.9
- first_gate: bfloat16 [4096, 12288], P('kv', 'tp'), may hold values from -0.09375 to 0.09375
- first_up: bfloat16 [4096, 12288], P('kv', 'tp'), may hold values from -0.09375 to 0.09375
- first_down: bfloat16 [12288, 4096], P('tp', 'kv'), may hold values from -0.078125 to 0.078125
- mixer_gain: float32 [4096], replicated, may hold values from 0.1 to 1.9
- query_weight: bfloat16 [4096, 2048], P(None, 'tp'), may hold values from -0.09375 to 0.09375
- key_weight: bfloat16 [4096, 2048], P(None, 'tp'), may hold values from -0.09375 to 0.09375
- value_weight: bfloat16 [4096, 4096], P(None, 'tp'), may hold values from -0.09375 to 0.09375
- input_weight: bfloat16 [4096, 16], replicated, may hold values from -0.09375 to 0.09375
- forget_weight: bfloat16 [4096, 16], replicated, may hold values from -0.09375 to 0.09375
- forget_bias: float32 [16], P('tp'), may hold values from -2 to 4
- output_weight: bfloat16 [4096, 4096], P('tp'), may hold values from -0.09375 to 0.09375
- last_gain: float32 [4096], replicated, may hold values from 0.1 to 1.9
- last_gate: bfloat16 [4096, 12288], P('kv', 'tp'), may hold values from -0.09375 to 0.09375
- last_up: bfloat16 [4096, 12288], P('kv', 'tp'), may hold values from -0.09375 to 0.09375
- last_down: bfloat16 [12288, 4096], P('tp', 'kv'), may hold values from -0.078125 to 0.078125
Outputs:
- result: bfloat16 [64, 4096], P(None, ('kv', 'tp'))
- new_memory: float32 [64, 16, 256, 128], P('kv', 'tp')
- new_normalizer: float32 [64, 16, 128], P('kv', 'tp')
- new_stabilizer: float32 [64, 16], P('kv', 'tp')
The draws below stay inside these ranges and needn't reach their ends.
All inputs are finite; a program needn't handle non-finite values.
Results may differ from the reference program's by a relative error of at most 0.025.
Values may be sent and summed in bfloat16 or wider, within the bound.
No kernel may reach another device: no remote copies, remote signals or barrier semaphores. Data moves between devices by JAX's collectives and lax.ppermute only.
A program may use at most 128 MiB of HBM per device.

```python
import jax
import jax.numpy as jnp
from jax import lax

D = 4096
FF = 12288
HEADS = 16
DK = 128
DV = 256
BATCH = 64


def strengthened(entries, own_key, source, target, blocks, factor):
    def block_of(dim):
        return (jnp.arange(entries.shape[dim]) // (entries.shape[dim] // blocks)).reshape((-1,) + (1,) * (entries.ndim - 1 - dim))

    first = jax.random.permutation(own_key, blocks)[block_of(target)]
    other_side = (block_of(target) + blocks // 2) % blocks
    return jnp.where((block_of(source) == first) | (block_of(source) == other_side), factor * entries, entries)


def block_scale(key, extent, cuts, smallest, top_value):
    def one(axis_at, blocks):
        heights = jax.random.uniform(jax.random.fold_in(jax.random.fold_in(key, 6), axis_at), (blocks,), jnp.float32, smallest / len(cuts), top_value / len(cuts))
        return jnp.repeat(jnp.exp(heights), extent[axis_at] // blocks).reshape((-1,) + (1,) * (len(extent) - axis_at - 1))

    loudness = one(*cuts[0])
    for cut in cuts[1:]:
        loudness = loudness * one(*cut)
    return loudness


def normal_values(own_key, shape, deviation, most, pieces=(), held_as=jnp.bfloat16):
    level = block_scale(own_key, shape, pieces, -0.22, 0.18) if pieces else 1.0
    drawn = jax.random.normal(own_key, shape, jnp.float32) * deviation * level
    return jnp.minimum(jnp.maximum(drawn, -most), most).astype(held_as)


def gaussian_with(stream_key, dims, spread, reach, cuts, heavy, dtype=jnp.bfloat16):
    values = spread * jax.random.normal(stream_key, dims, jnp.float32)
    if cuts:
        values = values * block_scale(stream_key, dims, cuts, -0.22, 0.18)
    return jnp.clip(strengthened(values, jax.random.fold_in(stream_key, 3), *heavy), -reach, reach).astype(dtype)


def setup_inputs(seed: int = 0) -> dict:
    arg_keys = jax.random.split(jax.random.key(seed), 21)
    tokens = normal_values(arg_keys[0], (BATCH, D), 1.0, 6.0, ((1, 32),))
    memory = normal_values(arg_keys[1], (BATCH, HEADS, DV, DK), 1.0, 6.0, ((0, 4), (1, 8)), jnp.float32)
    normalizer = normal_values(arg_keys[2], (BATCH, HEADS, DK), 1.0, 6.0, ((0, 4), (1, 8)), jnp.float32)
    stabilizer = normal_values(arg_keys[3], (BATCH, HEADS), 1.0, 4.0, ((0, 4), (1, 8)), jnp.float32)
    first_gain = jnp.clip(1.0 + 0.18 * jax.random.normal(arg_keys[4], (D,), jnp.float32), 0.1, 1.9)
    first_gate = normal_values(arg_keys[5], (D, FF), D ** -0.5, 0.09375, ((0, 4), (1, 8)))
    first_up = normal_values(arg_keys[6], (D, FF), D ** -0.5, 0.09375, ((0, 4), (1, 8)))
    first_down = gaussian_with(arg_keys[7], (FF, D), FF ** -0.5, 0.078125, ((0, 8), (1, 4)), (0, 1, 8, 2.0))
    mixer_gain = jnp.clip(1.0 + 0.18 * jax.random.normal(arg_keys[8], (D,), jnp.float32), 0.1, 1.9)
    query_weight = normal_values(arg_keys[9], (D, HEADS * DK), D ** -0.5, 0.09375, ((1, 8),))
    key_weight = normal_values(arg_keys[10], (D, HEADS * DK), D ** -0.5, 0.09375, ((1, 8),))
    value_weight = normal_values(arg_keys[11], (D, HEADS * DV), D ** -0.5, 0.09375, ((1, 8),))
    input_weight = normal_values(arg_keys[12], (D, HEADS), D ** -0.5, 0.09375)
    forget_weight = normal_values(arg_keys[13], (D, HEADS), D ** -0.5, 0.09375)
    forget_bias = jnp.clip(-2.0 + 6.0 * jax.random.uniform(arg_keys[14], (HEADS,), jnp.float32) ** block_scale(arg_keys[14], (HEADS,), ((0, 8),), -0.2, 0.2), -2.0, 4.0)
    output_weight = normal_values(arg_keys[15], (HEADS * DV, D), (HEADS * DV) ** -0.5, 0.09375, ((0, 8),))
    last_gain = jnp.clip(1.0 + 0.18 * jax.random.normal(arg_keys[16], (D,), jnp.float32), 0.1, 1.9)
    last_gate = normal_values(arg_keys[17], (D, FF), D ** -0.5, 0.09375, ((0, 4), (1, 8)))
    last_up = normal_values(arg_keys[18], (D, FF), D ** -0.5, 0.09375, ((0, 4), (1, 8)))
    last_down = gaussian_with(arg_keys[19], (FF, D), FF ** -0.5, 0.078125, ((0, 8), (1, 4)), (0, 1, 8, 2.0))
    return {"tokens": tokens, "memory": memory, "normalizer": normalizer, "stabilizer": stabilizer, "first_gain": first_gain, "first_gate": first_gate, "first_up": first_up, "first_down": first_down, "mixer_gain": mixer_gain, "query_weight": query_weight, "key_weight": key_weight, "value_weight": value_weight, "input_weight": input_weight, "forget_weight": forget_weight, "forget_bias": forget_bias, "output_weight": output_weight, "last_gain": last_gain, "last_gate": last_gate, "last_up": last_up, "last_down": last_down}


EPS = 1e-06

def norm_scale(stream):
    values = stream.astype(jnp.float32)
    return lax.rsqrt(lax.optimization_barrier(jnp.mean(values * values, axis=-1, keepdims=True)) + EPS)

def gated_mlp(stream, gain, w_gate, w_up, w_down):
    scale = norm_scale(stream)
    scaled = (stream.astype(jnp.float32) * gain).astype(jnp.bfloat16)
    gate = scale * jnp.dot(scaled, w_gate, preferred_element_type=jnp.float32)
    up = scale * jnp.dot(scaled, w_up, preferred_element_type=jnp.float32)
    hidden = (jax.nn.silu(gate) * up).astype(jnp.bfloat16)
    return jnp.dot(hidden, w_down, preferred_element_type=jnp.float32)

def reference(tokens, memory, normalizer, stabilizer, first_gain, first_gate, first_up, first_down, mixer_gain, query_weight, key_weight, value_weight, input_weight, forget_weight, forget_bias, output_weight, last_gain, last_gate, last_up, last_down):
    f32 = jnp.float32
    first_sum = gated_mlp(tokens, first_gain, first_gate, first_up, first_down)
    stream_one = (tokens.astype(f32) + 0.5 * first_sum).astype(jnp.bfloat16)
    batch = tokens.shape[0]
    scale = norm_scale(stream_one)
    cell_in = (stream_one.astype(f32) * mixer_gain).astype(jnp.bfloat16)
    query = (scale * jnp.dot(cell_in, query_weight, preferred_element_type=f32) * DK ** (-0.5)).reshape(batch, HEADS, DK)
    key = (scale * jnp.dot(cell_in, key_weight, preferred_element_type=f32)).reshape(batch, HEADS, DK)
    value = (scale * jnp.dot(cell_in, value_weight, preferred_element_type=f32)).reshape(batch, HEADS, DV)
    input_pre = scale * jnp.dot(cell_in, input_weight, preferred_element_type=f32)
    log_forget = jax.nn.log_sigmoid(scale * jnp.dot(cell_in, forget_weight, preferred_element_type=f32) + forget_bias)
    carried = log_forget + stabilizer
    new_stabilizer = jnp.maximum(carried, input_pre)
    keep = jnp.exp(carried - new_stabilizer)
    admit = jnp.exp(input_pre - new_stabilizer)
    recalled = jnp.einsum('bhvd,bhd->bhv', memory, query, precision=lax.Precision.HIGHEST)
    match = lax.optimization_barrier(jnp.sum(query * key, axis=-1))
    numer = keep[..., None] * recalled + (admit * match)[..., None] * value
    denom = keep * lax.optimization_barrier(jnp.sum(normalizer * query, axis=-1)) + admit * match
    cell_out = (numer / jnp.maximum(jnp.abs(denom), 1.0)[..., None]).reshape(batch, HEADS * DV).astype(jnp.bfloat16)
    new_memory = keep[..., None, None] * memory + admit[..., None, None] * value[..., :, None] * key[..., None, :]
    new_normalizer = keep[..., None] * normalizer + admit[..., None] * key
    mixed = jnp.dot(cell_out, output_weight, preferred_element_type=f32)
    stream_two = (stream_one.astype(f32) + mixed).astype(jnp.bfloat16)
    last_sum = gated_mlp(stream_two, last_gain, last_gate, last_up, last_down)
    result = (stream_two.astype(f32) + 0.5 * last_sum).astype(jnp.bfloat16)
    return (result, new_memory, new_normalizer, new_stabilizer)
```

```python
import jax
import jax.numpy as jnp
from jax import lax
from jax.sharding import PartitionSpec as P

EPS = 1e-06
LANES = 128
F32 = jnp.float32
BF16 = jnp.bfloat16


def shifts(axis):
    size = lax.axis_size(axis)
    return [[(s, (s + d) % size) for s in range(size)] for d in range(1, size)]


def sum_rows_scattered(parts, axis):
    size = lax.axis_size(axis)
    me = lax.axis_index(axis)
    if size > 4:
        got = lax.all_to_all(parts, axis, split_axis=0, concat_axis=0, tiled=True)
        return jnp.sum(got.astype(F32), axis=0)
    total = lax.dynamic_index_in_dim(parts, me, 0, keepdims=False).astype(F32)
    for d, perm in enumerate(shifts(axis), 1):
        piece = lax.dynamic_index_in_dim(parts, (me + d) % size, 0, keepdims=False)
        total = total + lax.ppermute(piece, axis, perm).astype(F32)
    return total


def gather_rows(piece, axis):
    size = lax.axis_size(axis)
    me = lax.axis_index(axis)
    rows = piece.shape[0]
    if size > 4:
        return gather_blocks(piece, axis).reshape(size * rows, piece.shape[1])
    whole = jnp.zeros((size * rows, piece.shape[1]), piece.dtype)
    whole = lax.dynamic_update_slice_in_dim(whole, piece, me * rows, 0)
    for d, perm in enumerate(shifts(axis), 1):
        got = lax.ppermute(piece, axis, perm)
        whole = lax.dynamic_update_slice_in_dim(whole, got, ((me - d) % size) * rows, 0)
    return whole


def gather_blocks(piece, axis):
    size = lax.axis_size(axis)
    return lax.all_to_all(
        jnp.broadcast_to(piece[None], (size,) + piece.shape), axis, 0, 0, tiled=True
    )


def side_by_side(blocks):
    count, rows, cols = blocks.shape
    return jnp.transpose(blocks, (1, 0, 2)).reshape(rows, count * cols)


def apart(whole, count):
    rows, cols = whole.shape
    return jnp.transpose(whole.reshape(rows, count, cols // count), (1, 0, 2))


def gated_share(block, gain, w_gate, w_up, w_down, model_width):
    groups = lax.axis_size("kv")
    rows, width = block.shape
    units = w_gate.shape[1]
    gain_block = lax.dynamic_slice_in_dim(gain, lax.axis_index("kv") * width, width, 0)
    values = block.astype(F32)
    scaled = (values * gain_block).astype(BF16)
    gate = jnp.dot(scaled, w_gate, preferred_element_type=F32).astype(BF16)
    up = jnp.dot(scaled, w_up, preferred_element_type=F32).astype(BF16)
    squares = jnp.sum(values * values, axis=1, keepdims=True)
    high = squares.astype(BF16)
    low = (squares - high.astype(F32)).astype(BF16)
    tail = jnp.concatenate([high, low, jnp.zeros((rows, LANES - 2), BF16)], axis=1)
    parts = jnp.concatenate([gate, up, tail], axis=1).reshape(groups, rows // groups, -1)
    total = sum_rows_scattered(parts, "kv")
    sq = total[:, 2 * units : 2 * units + 1] + total[:, 2 * units + 1 : 2 * units + 2]
    scale = lax.rsqrt(sq / model_width + EPS)
    piece = (jax.nn.silu(scale * total[:, :units]) * (scale * total[:, units : 2 * units])).astype(BF16)
    hidden = gather_rows(piece, "kv")
    sums = jnp.dot(hidden, w_down, preferred_element_type=F32).astype(BF16)
    got = lax.all_to_all(apart(sums, lax.axis_size("tp")), "tp", 0, 0, tiled=True)
    return jnp.sum(got.astype(F32), axis=0)


def body(
    tokens,
    memory,
    normalizer,
    stabilizer,
    first_gain,
    first_gate,
    first_up,
    first_down,
    mixer_gain,
    query_weight,
    key_weight,
    value_weight,
    input_weight,
    forget_weight,
    forget_bias,
    output_weight,
    last_gain,
    last_gate,
    last_up,
    last_down,
):
    model_width = first_gain.shape[0]
    rows, col_width = tokens.shape
    groups, members = lax.axis_size("kv"), lax.axis_size("tp")
    seq_count, head_count, value_size, key_size = memory.shape
    block = side_by_side(gather_blocks(tokens, "tp"))
    share = gated_share(block, first_gain, first_gate, first_up, first_down, model_width)
    stream_one = (tokens.astype(F32) + 0.5 * share).astype(BF16)
    spread = jnp.broadcast_to(
        stream_one.reshape(groups, 1, seq_count, col_width),
        (groups, members, seq_count, col_width),
    ).reshape(groups * members, seq_count, col_width)
    own_rows = side_by_side(lax.all_to_all(spread, ("kv", "tp"), 0, 0, tiled=True))
    row_values = own_rows.astype(F32)
    scale = lax.rsqrt(jnp.mean(row_values * row_values, axis=1, keepdims=True) + EPS)
    cell_in = (row_values * mixer_gain).astype(BF16)
    query = (
        scale * jnp.dot(cell_in, query_weight, preferred_element_type=F32) * key_size ** (-0.5)
    ).reshape(seq_count, head_count, key_size)
    key = (scale * jnp.dot(cell_in, key_weight, preferred_element_type=F32)).reshape(
        seq_count, head_count, key_size
    )
    value = (scale * jnp.dot(cell_in, value_weight, preferred_element_type=F32)).reshape(
        seq_count, head_count, value_size
    )
    first_head = lax.axis_index("tp") * head_count
    gates = scale * jnp.dot(
        cell_in,
        jnp.concatenate(
            [
                lax.dynamic_slice_in_dim(input_weight, first_head, head_count, 1),
                lax.dynamic_slice_in_dim(forget_weight, first_head, head_count, 1),
            ],
            axis=1,
        ),
        preferred_element_type=F32,
    )
    input_pre = gates[:, :head_count]
    log_forget = jax.nn.log_sigmoid(gates[:, head_count:] + forget_bias)
    carried = log_forget + stabilizer
    new_stabilizer = jnp.maximum(carried, input_pre)
    keep = jnp.exp(carried - new_stabilizer)
    admit = jnp.exp(input_pre - new_stabilizer)
    recalled = jnp.sum(memory * query[:, :, None, :], axis=-1)
    match = jnp.sum(query * key, axis=-1)
    numer = keep[..., None] * recalled + (admit * match)[..., None] * value
    denom = keep * jnp.sum(normalizer * query, axis=-1) + admit * match
    cell_out = (
        (numer / jnp.maximum(jnp.abs(denom), 1.0)[..., None])
        .reshape(seq_count, head_count * value_size)
        .astype(BF16)
    )
    new_memory = (
        keep[..., None, None] * memory
        + admit[..., None, None] * value[..., :, None] * key[..., None, :]
    )
    new_normalizer = keep[..., None] * normalizer + admit[..., None] * key
    mixed_part = jnp.dot(cell_out, output_weight, preferred_element_type=F32).astype(BF16)
    pieces = jnp.transpose(
        mixed_part.reshape(seq_count, groups, members, col_width), (2, 1, 0, 3)
    )
    got = lax.all_to_all(pieces, "tp", 0, 0, tiled=True)
    mixed = jnp.sum(got.astype(F32), axis=0)
    held = jnp.transpose(own_rows.reshape(seq_count, groups, members, col_width), (2, 1, 0, 3))
    mine = lax.dynamic_index_in_dim(held, lax.axis_index("tp"), 0, keepdims=False)
    rows_two = (mine.astype(F32) + mixed).astype(BF16)
    spread = jnp.broadcast_to(
        rows_two[:, None], (groups, members, seq_count, col_width)
    ).reshape(groups * members, seq_count, col_width)
    got = lax.all_to_all(spread, ("kv", "tp"), 0, 0, tiled=True)
    whole_two = jnp.transpose(
        got.reshape(groups, members, seq_count, col_width), (0, 2, 1, 3)
    ).reshape(rows, members * col_width)
    last_share = gated_share(whole_two, last_gain, last_gate, last_up, last_down, model_width)
    own_columns = lax.dynamic_index_in_dim(
        got.reshape(groups, members, seq_count, col_width), lax.axis_index("tp"), 1, keepdims=False
    ).reshape(rows, col_width)
    result = (own_columns.astype(F32) + 0.5 * last_share).astype(BF16)
    return (result, new_memory, new_normalizer, new_stabilizer)


def solution(mesh):
    in_specs = (
        P(None, ("kv", "tp")),
        P("kv", "tp", None, None),
        P("kv", "tp", None),
        P("kv", "tp"),
        P(),
        P("kv", "tp"),
        P("kv", "tp"),
        P("tp", "kv"),
        P(),
        P(None, "tp"),
        P(None, "tp"),
        P(None, "tp"),
        P(),
        P(),
        P("tp"),
        P("tp", None),
        P(),
        P("kv", "tp"),
        P("kv", "tp"),
        P("tp", "kv"),
    )
    out_specs = (
        P(None, ("kv", "tp")),
        P("kv", "tp", None, None),
        P("kv", "tp", None),
        P("kv", "tp"),
    )
    return jax.shard_map(body, mesh=mesh, in_specs=in_specs, out_specs=out_specs, check_vma=False)
```

```python
import jax
import jax.numpy as jnp
from jax import lax
from jax.experimental import pallas as pl
from jax.experimental.pallas import tpu as pltpu
from jax.sharding import PartitionSpec as P

EPS = 1e-06
LANES = 128
F32 = jnp.float32
BF16 = jnp.bfloat16


def shifts(axis):
    size = lax.axis_size(axis)
    return [[(s, (s + d) % size) for s in range(size)] for d in range(1, size)]


def sum_rows_scattered(parts, axis):
    size = lax.axis_size(axis)
    me = lax.axis_index(axis)
    if size > 4:
        got = lax.all_to_all(parts, axis, split_axis=0, concat_axis=0, tiled=True)
        return jnp.sum(got.astype(F32), axis=0)
    total = lax.dynamic_index_in_dim(parts, me, 0, keepdims=False).astype(F32)
    for d, perm in enumerate(shifts(axis), 1):
        piece = lax.dynamic_index_in_dim(parts, (me + d) % size, 0, keepdims=False)
        total = total + lax.ppermute(piece, axis, perm).astype(F32)
    return total


def gather_rows(piece, axis):
    size = lax.axis_size(axis)
    me = lax.axis_index(axis)
    rows = piece.shape[0]
    if size > 4:
        return gather_blocks(piece, axis).reshape(size * rows, piece.shape[1])
    whole = jnp.zeros((size * rows, piece.shape[1]), piece.dtype)
    whole = lax.dynamic_update_slice_in_dim(whole, piece, me * rows, 0)
    for d, perm in enumerate(shifts(axis), 1):
        got = lax.ppermute(piece, axis, perm)
        whole = lax.dynamic_update_slice_in_dim(whole, got, ((me - d) % size) * rows, 0)
    return whole


def gather_blocks(piece, axis):
    size = lax.axis_size(axis)
    return lax.all_to_all(
        jnp.broadcast_to(piece[None], (size,) + piece.shape), axis, 0, 0, tiled=True
    )


def core():
    return lax.axis_index("tp") % 2


def layer():
    return lax.axis_index("tp") // 2


def layers():
    return lax.axis_size("tp") // 2


def layer_groups():
    return [[2 * z + c for z in range(layers())] for c in range(2)]


def column_groups():
    members = lax.axis_size("tp")
    return [
        [k * members + 2 * z + c for k in range(lax.axis_size("kv")) for z in range(layers())]
        for c in range(2)
    ]


def swap_cores(x):
    return lax.ppermute(x, "tp", [(s, s ^ 1) for s in range(lax.axis_size("tp"))])


def over_layer(x, d):
    return lax.ppermute(x, "tp", [(s, s ^ (2 * d)) for s in range(lax.axis_size("tp"))])


def both_cores(mine):
    other = swap_cores(mine)
    first = core() == 0
    return jnp.where(first, mine, other), jnp.where(first, other, mine)


def gather_members(piece):
    if layers() > 4:
        return side_by_side(gather_blocks(piece, "tp"))
    got = jnp.zeros((layers(),) + piece.shape, piece.dtype)
    got = lax.dynamic_update_index_in_dim(got, piece, layer(), 0)
    for d in range(1, layers()):
        got = lax.dynamic_update_index_in_dim(got, over_layer(piece, d), layer() ^ d, 0)
    low, high = both_cores(got)
    return side_by_side(jnp.stack([low, high], axis=1).reshape((-1,) + piece.shape))


def sum_members_scattered(parts):
    if layers() > 4:
        got = lax.all_to_all(parts, "tp", 0, 0, tiled=True)
        return jnp.sum(got.astype(F32), axis=0)
    pairs = parts.reshape((layers(), 2) + parts.shape[1:])
    theirs = lax.dynamic_index_in_dim(pairs, 1 - core(), 1, keepdims=False)
    ours = lax.dynamic_index_in_dim(pairs, core(), 1, keepdims=False).astype(F32)
    ours = ours + swap_cores(theirs).astype(F32)
    sent = ours.astype(BF16)
    total = lax.dynamic_index_in_dim(ours, layer(), 0, keepdims=False)
    for d in range(1, layers()):
        piece = lax.dynamic_index_in_dim(sent, layer() ^ d, 0, keepdims=False)
        total = total + over_layer(piece, d).astype(F32)
    return total


def exchange_columns(half):
    groups = lax.axis_size("kv")
    spread = jnp.broadcast_to(
        half[:, None], (groups, layers()) + half.shape[1:]
    ).reshape((groups * layers(),) + half.shape[1:])
    got = lax.all_to_all(spread, ("kv", "tp"), 0, 0, axis_index_groups=column_groups())
    total = jnp.sum(got.reshape((groups, layers()) + half.shape[1:]).astype(F32), axis=1)
    return both_cores(total.astype(BF16))


def side_by_side(blocks):
    count, rows, cols = blocks.shape
    return jnp.transpose(blocks, (1, 0, 2)).reshape(rows, count * cols)


def apart(whole, count):
    rows, cols = whole.shape
    return jnp.transpose(whole.reshape(rows, count, cols // count), (1, 0, 2))


def cuts(extent, count):
    step = extent // count
    if extent % count or step % LANES:
        return [(0, extent)]
    return [(i * step, step) for i in range(count)]


def params():
    return pltpu.CompilerParams(vmem_limit_bytes=48 * 1024 * 1024)


ANY = pl.BlockSpec(memory_space=pl.ANY)
VMEM = pl.BlockSpec(memory_space=pltpu.VMEM)


def gate_up(block, gain_block, w_gate, w_up):
    rows, width = block.shape
    units = w_gate.shape[1]
    pieces = cuts(units, 4)

    def kernel(x_ref, gain_ref, gate_hbm, up_hbm, out_ref, gate_buf, up_buf, sems):
        copies = []
        for i, (at, size) in enumerate(pieces):
            for j, (src, dst) in enumerate(((gate_hbm, gate_buf), (up_hbm, up_buf))):
                copy = pltpu.make_async_copy(
                    src.at[:, pl.ds(at, size)], dst.at[:, pl.ds(at, size)], sems.at[i, j]
                )
                copy.start()
                copies.append((copy, dst, at, size, j * units + at))
        values = x_ref[...].astype(F32)
        scaled = (values * gain_ref[...]).astype(BF16)
        squares = jnp.sum(values * values, axis=1, keepdims=True)
        high = squares.astype(BF16).astype(F32)
        lane = lax.broadcasted_iota(jnp.int32, (rows, LANES), 1)
        tail = jnp.where(lane == 0, high, jnp.where(lane == 1, squares - high, 0.0))
        out_ref[:, pl.ds(2 * units, LANES)] = tail.astype(BF16)
        for copy, buf, at, size, to in copies:
            copy.wait()
            acc = jnp.dot(scaled, buf[:, pl.ds(at, size)], preferred_element_type=F32)
            out_ref[:, pl.ds(to, size)] = acc.astype(BF16)

    return pl.pallas_call(
        kernel,
        out_shape=jax.ShapeDtypeStruct((rows, 2 * units + LANES), BF16),
        in_specs=[VMEM, VMEM, ANY, ANY],
        out_specs=VMEM,
        scratch_shapes=[
            pltpu.VMEM((width, units), BF16),
            pltpu.VMEM((width, units), BF16),
            pltpu.SemaphoreType.DMA((len(pieces), 2)),
        ],
        compiler_params=params(),
        name="gate_up",
    )(block, gain_block, w_gate, w_up)


def down(hidden, w_down, count):
    rows, units = hidden.shape
    width = w_down.shape[1]
    part = width // count
    pieces = cuts(width, 4)

    def kernel(x_ref, w_hbm, out_ref, buf, sems):
        copies = []
        for i, (at, size) in enumerate(pieces):
            copy = pltpu.make_async_copy(
                w_hbm.at[:, pl.ds(at, size)], buf.at[:, pl.ds(at, size)], sems.at[i]
            )
            copy.start()
            copies.append(copy)
        for copy, (at, size) in zip(copies, pieces):
            copy.wait()
            acc = jnp.dot(x_ref[...], buf[:, pl.ds(at, size)], preferred_element_type=F32)
            acc = acc.astype(BF16)
            for off in range(0, size, min(part, size)):
                step = min(part, size)
                out_ref[(at + off) // part, :, pl.ds((at + off) % part, step)] = acc[
                    :, off : off + step
                ]

    return pl.pallas_call(
        kernel,
        out_shape=jax.ShapeDtypeStruct((count, rows, part), BF16),
        in_specs=[VMEM, ANY],
        out_specs=VMEM,
        scratch_shapes=[pltpu.VMEM((units, width), BF16), pltpu.SemaphoreType.DMA((len(pieces),))],
        compiler_params=params(),
        name="down",
    )(hidden, w_down)


def cell(own_rows, gain, w_query, w_key, w_value, w_gates, w_out, bias, memory, normalizer, stabilizer, groups):
    seqs, model = own_rows.shape
    _, heads, dv, dk = memory.shape
    half = model // (2 * groups)
    steps = cuts(model, 4)
    seq_steps = [(i * (seqs // 4), seqs // 4) for i in range(4)] if seqs % 4 == 0 else [(0, seqs)]
    out_steps = cuts(model, 4)

    def kernel(
        x_ref, gain_ref, gates_ref, bias_ref, norm_ref, stab_ref,
        q_hbm, k_hbm, v_hbm, out_hbm, mem_hbm,
        part_ref, key_ref, value_ref, keep_ref, admit_ref, norm_out, stab_out,
        q_buf, k_buf, v_buf, out_buf, mem_buf, w_sems, mem_sems, out_sems,
    ):
        w_copies, mem_copies, out_copies = [], [], []
        for i, (at, size) in enumerate(steps):
            for j, (src, dst) in enumerate(((q_hbm, q_buf), (k_hbm, k_buf), (v_hbm, v_buf))):
                w_copies.append(
                    pltpu.make_async_copy(
                        src.at[pl.ds(at, size)], dst.at[pl.ds(at, size)], w_sems.at[i, j]
                    )
                )
        for i, (at, size) in enumerate(seq_steps):
            mem_copies.append(
                pltpu.make_async_copy(
                    mem_hbm.at[pl.ds(at, size)], mem_buf.at[pl.ds(at, size)], mem_sems.at[i]
                )
            )
        for i, (at, size) in enumerate(out_steps):
            out_copies.append(
                pltpu.make_async_copy(
                    out_hbm.at[:, pl.ds(at, size)], out_buf.at[:, pl.ds(at, size)], out_sems.at[i]
                )
            )
        for copy in w_copies + mem_copies + out_copies:
            copy.start()
        values = x_ref[...].astype(F32)
        scale = lax.rsqrt(jnp.mean(values * values, axis=1, keepdims=True) + EPS)
        cell_in = (values * gain_ref[...]).astype(BF16)
        gates = scale * lax.dot_general(
            cell_in, gates_ref[...], (((1,), (1,)), ((), ())), preferred_element_type=F32
        )
        sums = [0.0, 0.0, 0.0]
        for i, (at, size) in enumerate(steps):
            for j, buf in enumerate((q_buf, k_buf, v_buf)):
                w_copies[3 * i + j].wait()
                sums[j] = sums[j] + jnp.dot(
                    cell_in[:, at : at + size], buf[pl.ds(at, size)], preferred_element_type=F32
                )
        query = scale * sums[0] * dk ** (-0.5)
        key = scale * sums[1]
        value = scale * sums[2]
        key_ref[...] = key
        value_ref[...] = value
        input_pre = gates[:, :heads]
        carried = jax.nn.log_sigmoid(gates[:, heads : 2 * heads] + bias_ref[...]) + stab_ref[...]
        stabil = jnp.maximum(carried, input_pre)
        keep = jnp.exp(carried - stabil)
        admit = jnp.exp(input_pre - stabil)
        stab_out[...] = stabil
        keep_ref[...] = keep
        admit_ref[...] = admit
        norms = norm_ref[...]
        asked = query.astype(BF16)
        recalled = [jnp.zeros((seqs, dv), F32) for _ in range(heads)]
        row = lax.broadcasted_iota(jnp.int32, (seqs, dv), 0)
        for copy, (at, size) in zip(mem_copies, seq_steps):
            copy.wait()
            for b in range(at, at + size):
                for h in range(heads):
                    got = lax.dot_general(
                        asked[:, h * dk : (h + 1) * dk],
                        mem_buf[b, h].astype(BF16),
                        (((1,), (1,)), ((), ())),
                        preferred_element_type=F32,
                    )
                    recalled[h] = jnp.where(row == b, got, recalled[h])
        outs = []
        for h in range(heads):
            lanes = slice(h * dk, (h + 1) * dk)
            q, k, n = query[:, lanes], key[:, lanes], norms[:, lanes]
            kept, let = keep[:, h : h + 1], admit[:, h : h + 1]
            matched = let * jnp.sum(q * k, axis=1, keepdims=True)
            numer = kept * recalled[h] + matched * value[:, h * dv : (h + 1) * dv]
            denom = kept * jnp.sum(n * q, axis=1, keepdims=True) + matched
            outs.append((numer / jnp.maximum(jnp.abs(denom), 1.0)).astype(BF16))
            norm_out[:, pl.ds(h * dk, dk)] = kept * n + let * k
        cell_out = jnp.concatenate(outs, axis=1)
        for copy, (at, size) in zip(out_copies, out_steps):
            copy.wait()
            acc = jnp.dot(cell_out, out_buf[:, pl.ds(at, size)], preferred_element_type=F32)
            acc = acc.astype(BF16)
            for off in range(0, size, half):
                which = (at + off) // half
                part_ref[which % 2, which // 2] = acc[:, off : off + half]

    shape = jax.ShapeDtypeStruct
    return pl.pallas_call(
        kernel,
        out_shape=(
            shape((2, groups, seqs, half), BF16),
            shape((seqs, heads * dk), F32),
            shape((seqs, heads * dv), F32),
            shape((seqs, heads), F32),
            shape((seqs, heads), F32),
            shape((seqs, heads * dk), F32),
            shape((seqs, heads), F32),
        ),
        in_specs=[VMEM] * 6 + [ANY] * 5,
        out_specs=(VMEM,) * 7,
        scratch_shapes=[
            pltpu.VMEM(w_query.shape, BF16),
            pltpu.VMEM(w_key.shape, BF16),
            pltpu.VMEM(w_value.shape, BF16),
            pltpu.VMEM(w_out.shape, BF16),
            pltpu.VMEM(memory.shape, F32),
            pltpu.SemaphoreType.DMA((len(steps), 3)),
            pltpu.SemaphoreType.DMA((len(seq_steps),)),
            pltpu.SemaphoreType.DMA((len(out_steps),)),
        ],
        compiler_params=params(),
        name="cell",
    )(
        own_rows, gain[None], w_gates, bias[None], normalizer.reshape(seqs, heads * dk), stabilizer,
        w_query, w_key, w_value, w_out, memory,
    )


def gated_part(block, gain, w_gate, w_up, w_down, model_width, count):
    groups = lax.axis_size("kv")
    rows, width = block.shape
    units = w_gate.shape[1]
    gain_block = lax.dynamic_slice_in_dim(gain, lax.axis_index("kv") * width, width, 0)
    parts = gate_up(block, gain_block[None], w_gate, w_up).reshape(groups, rows // groups, -1)
    total = sum_rows_scattered(parts, "kv")
    sq = total[:, 2 * units : 2 * units + 1] + total[:, 2 * units + 1 : 2 * units + 2]
    scale = lax.rsqrt(sq / model_width + EPS)
    piece = (jax.nn.silu(scale * total[:, :units]) * (scale * total[:, units : 2 * units])).astype(BF16)
    return down(gather_rows(piece, "kv"), w_down, count)


def body(
    tokens,
    memory,
    normalizer,
    stabilizer,
    first_gain,
    first_gate,
    first_up,
    first_down,
    mixer_gain,
    query_weight,
    key_weight,
    value_weight,
    input_weight,
    forget_weight,
    forget_bias,
    output_weight,
    last_gain,
    last_gate,
    last_up,
    last_down,
):
    model_width = first_gain.shape[0]
    rows, col_width = tokens.shape
    groups, members = lax.axis_size("kv"), lax.axis_size("tp")
    seq_count, head_count, value_size, key_size = memory.shape
    width = members * col_width
    half = width // 2
    leads = (layer() == 0).astype(F32)
    block = gather_members(tokens)
    part = gated_part(block, first_gain, first_gate, first_up, first_down, model_width, 2)
    theirs = lax.dynamic_index_in_dim(part, 1 - core(), 0, keepdims=False)
    ours = lax.dynamic_index_in_dim(part, core(), 0, keepdims=False).astype(F32)
    held = lax.dynamic_slice_in_dim(block, core() * half, half, 1).astype(F32)
    ours = 0.5 * (ours + swap_cores(theirs).astype(F32)) + leads * held
    low, high = exchange_columns(ours.astype(BF16).reshape(groups, seq_count, half))
    own_rows = side_by_side(jnp.concatenate([low, high], axis=2))
    first_head = lax.axis_index("tp") * head_count
    w_gates = jnp.concatenate(
        [
            lax.dynamic_slice_in_dim(input_weight.T, first_head, head_count, 0),
            lax.dynamic_slice_in_dim(forget_weight.T, first_head, head_count, 0),
            jnp.zeros((16 - 2 * head_count, model_width), BF16),
        ],
        axis=0,
    )
    pairs, key, value, keep, admit, new_normalizer, new_stabilizer = cell(
        own_rows, mixer_gain, query_weight, key_weight, value_weight, w_gates, output_weight,
        forget_bias, memory, normalizer, stabilizer, groups,
    )
    theirs = lax.dynamic_index_in_dim(pairs, 1 - core(), 0, keepdims=False)
    ours = lax.dynamic_index_in_dim(pairs, core(), 0, keepdims=False).astype(F32)
    held = lax.dynamic_index_in_dim(
        own_rows.reshape(seq_count, groups, 2, half), core(), 2, keepdims=False
    ).astype(F32)
    ours = ours + swap_cores(theirs).astype(F32) + leads * jnp.transpose(held, (1, 0, 2))
    ours, keep, admit, value, key = lax.optimization_barrier(
        (ours.astype(BF16), keep, admit, value, key)
    )
    low, high = exchange_columns(ours)
    value = value.reshape(seq_count, head_count, value_size, 1)
    key = key.reshape(seq_count, head_count, 1, key_size)
    new_memory = keep[..., None, None] * memory + admit[..., None, None] * value * key
    new_normalizer = new_normalizer.reshape(normalizer.shape)
    whole_two = jnp.concatenate([low, high], axis=2).reshape(rows, width)
    wide = layers() <= 4 and col_width % LANES == 0
    part = gated_part(
        whole_two, last_gain, last_gate, last_up, last_down, model_width, members if wide else 1
    )
    share = sum_members_scattered(part if wide else apart(part[0], members))
    own_columns = lax.dynamic_slice_in_dim(
        whole_two, lax.axis_index("tp") * col_width, col_width, 1
    )
    result = (own_columns.astype(F32) + 0.5 * share).astype(BF16)
    return (result, new_memory, new_normalizer, new_stabilizer)


def solution(mesh):
    in_specs = (
        P(None, ("kv", "tp")),
        P("kv", "tp", None, None),
        P("kv", "tp", None),
        P("kv", "tp"),
        P(),
        P("kv", "tp"),
        P("kv", "tp"),
        P("tp", "kv"),
        P(),
        P(None, "tp"),
        P(None, "tp"),
        P(None, "tp"),
        P(),
        P(),
        P("tp"),
        P("tp", None),
        P(),
        P("kv", "tp"),
        P("kv", "tp"),
        P("tp", "kv"),
    )
    out_specs = (
        P(None, ("kv", "tp")),
        P("kv", "tp", None, None),
        P("kv", "tp", None),
        P("kv", "tp"),
    )
    return jax.shard_map(body, mesh=mesh, in_specs=in_specs, out_specs=out_specs, check_vma=False)
```
